32 devices in a mesh: fs: 8 (over z, x), tp: 4 (over y, core).
Axes of the slice: x: 2, y: 2, z: 4, core: 2. Of those that a mesh axis runs over, the one named last changes fastest.
Arguments:
- x_late: bfloat16 [4096, 2048], P(('fs', 'tp')), may hold values from -6 to 6
- x_early: bfloat16 [4096, 2048], P(('fs', 'tp')), may hold values from -6 to 6
- d_hidden: bfloat16 [4096, 3072], P('fs', 'tp'), may hold values from -6 to 6
- w_gate: bfloat16 [2048, 3072], P('fs', 'tp'), may hold values from -0.125 to 0.125
- w_up: bfloat16 [2048, 3072], P('fs', 'tp'), may hold values from -0.125 to 0.125
- gate_sum: float32 [2048, 3072], P('fs', 'tp'), may hold values from -192 to 192
- up_sum: float32 [2048, 3072], P('fs', 'tp'), may hold values from -192 to 192
Outputs:
- hidden_late: bfloat16 [4096, 3072], P('fs', 'tp')
- grad_input: bfloat16 [4096, 2048], P(('fs', 'tp'))
- gate_sum_out: float32 [2048, 3072], P('fs', 'tp')
- up_sum_out: float32 [2048, 3072], P('fs', 'tp')
The draws below stay inside these ranges and needn't reach their ends.
All inputs are finite; a program needn't handle non-finite values.
Results may differ from the reference program's by a relative error of at most 0.0095.
Values may be sent and summed in bfloat16 or wider, within the bound.
A program may use at most 128 MiB of HBM per device.

```python
import jax
import jax.numpy as jnp
from jax import lax

D = 2048
FF = 3072
TOKENS = 4096
N_TP = 4


def with_spikes(result, rng, source, target, shards_of, factor):
    owner, partner = [(jnp.arange(result.shape[dim]) // (result.shape[dim] // shards_of)).reshape([-1 if axis == dim else 1 for axis in range(result.ndim)]) for dim in (source, target)]
    chosen = jax.random.permutation(rng, shards_of)[partner]
    strong = (owner == chosen) | (owner == (partner + shards_of // 2) % shards_of)
    return jnp.where(strong, factor * result, result)


def level_of(stream_key, extent, shards, least, largest):
    factor_of, own = 1.0, jax.random.fold_in(stream_key, 6)
    for axis_at, parts in shards:
        heights = jnp.exp(jax.random.uniform(jax.random.fold_in(own, axis_at), (parts,), jnp.float32, least / len(shards), largest / len(shards)))
        factor_of = factor_of * jnp.repeat(heights, extent[axis_at] // parts).reshape([-1 if axis == axis_at else 1 for axis in range(len(extent))])
    return factor_of


def gaussian(key, extent, spread, limit, shards=(), dtype=jnp.bfloat16):
    gain = level_of(key, extent, shards, -0.22, 0.18) if shards else 1.0
    entries = jax.random.normal(key, extent, jnp.float32) * spread * gain
    return jnp.minimum(jnp.maximum(entries, -limit), limit).astype(dtype)


def gaussian_with(own_key, dims, spread, most, cuts, heavy, held_as=jnp.bfloat16):
    entries = spread * jax.random.normal(own_key, dims, jnp.float32)
    if cuts:
        entries = entries * level_of(own_key, dims, cuts, -0.22, 0.18)
    return jnp.clip(with_spikes(entries, jax.random.fold_in(own_key, 3), *heavy), -most, most).astype(held_as)


def setup_inputs(seed: int = 0) -> dict:
    streams_of = jax.random.split(jax.random.key(seed), 8)
    return {
        "x_late": gaussian(streams_of[0], (TOKENS, D), 1.0, 6.0, ((0, 32),)),
        "x_early": gaussian_with(streams_of[1], (TOKENS, D), 1.0, 6.0, ((0, 32),), (0, 1, 32, 2.75)),
        "d_hidden": gaussian_with(streams_of[2], (TOKENS, FF), 1.0, 6.0, ((0, 8), (1, 4)), (0, 1, 8, 2.0)),
        "w_gate": gaussian(streams_of[3], (D, FF), D ** -0.5, 0.125, ((0, 8), (1, 4))),
        "w_up": gaussian(streams_of[4], (D, FF), D ** -0.5, 0.125, ((0, 8), (1, 4))),
        "gate_sum": gaussian(streams_of[5], (D, FF), (0.5 * TOKENS ** 0.5), 192.0, ((0, 8), (1, 4)), jnp.float32),
        "up_sum": gaussian(streams_of[6], (D, FF), (0.5 * TOKENS ** 0.5), 192.0, ((0, 8), (1, 4)), jnp.float32),
    }


def reference(x_late, x_early, d_hidden, w_gate, w_up, gate_sum, up_sum):
    gate_late = jnp.dot(x_late, w_gate, preferred_element_type=jnp.float32)
    up_late = jnp.dot(x_late, w_up, preferred_element_type=jnp.float32)
    sigmoid_late = jax.nn.sigmoid(gate_late)
    hidden_late = (gate_late * sigmoid_late * up_late).astype(jnp.bfloat16)
    gate_early = jnp.dot(x_early, w_gate, preferred_element_type=jnp.float32)
    up_early = jnp.dot(x_early, w_up, preferred_element_type=jnp.float32)
    sigmoid_early = jax.nn.sigmoid(gate_early)
    cotangent = d_hidden.astype(jnp.float32)
    d_gate = (cotangent * up_early * sigmoid_early * (1.0 + gate_early * (1.0 - sigmoid_early))).astype(jnp.bfloat16)
    d_up = (cotangent * gate_early * sigmoid_early).astype(jnp.bfloat16)
    span = FF // N_TP
    total = jnp.zeros((x_early.shape[0], x_early.shape[1]), jnp.float32)
    for index in range(N_TP):
        lower = index * span
        partial_value = jnp.dot(d_gate[:, lower:lower + span], w_gate[:, lower:lower + span].T, preferred_element_type=jnp.float32)
        partial_value = partial_value + jnp.dot(d_up[:, lower:lower + span], w_up[:, lower:lower + span].T, preferred_element_type=jnp.float32)
        rounded = lax.optimization_barrier(partial_value.astype(jnp.bfloat16))
        total = total + rounded.astype(jnp.float32)
    grad_input = total.astype(jnp.bfloat16)
    gate_sum_out = gate_sum + jnp.dot(x_early.T, d_gate, preferred_element_type=jnp.float32)
    up_sum_out = up_sum + jnp.dot(x_early.T, d_up, preferred_element_type=jnp.float32)
    return (hidden_late, grad_input, gate_sum_out, up_sum_out)
```

```python
import functools

import jax
import jax.numpy as jnp
from jax import lax
from jax.experimental import pallas as pl
from jax.experimental.pallas import tpu as pltpu
from jax.sharding import PartitionSpec as P

MESH = pl.DeviceIdType.MESH
F32 = jnp.float32
BF16 = jnp.bfloat16


def place(fs_count):
    fs, tp = lax.axis_index("fs"), lax.axis_index("tp")
    return lax.div(fs, 2), lax.rem(fs, 2), tp, fs_count // 2


def greet(devices):
    barrier = pltpu.get_barrier_semaphore()
    for device in devices:
        pl.semaphore_signal(barrier, inc=1, device_id=device, device_id_type=MESH)
    pl.semaphore_wait(barrier, len(devices))


def bits_of(tp_count):
    return [1 << b for b in range(tp_count.bit_length() - 1)]


def flip(tp, bit):
    return jnp.where(lax.rem(lax.div(tp, bit), 2) == 0, tp + bit, tp - bit)


def flips(tp, mask, bits):
    for bit in bits:
        if mask & bit:
            tp = flip(tp, bit)
    return tp


class Copies:
    def __init__(self, send_sem, recv_sem):
        self.send_sem, self.recv_sem = send_sem, recv_sem
        self.made, self.waited = {}, set()

    def start(self, key, src, dst, device):
        index = len(self.made)
        copy = pltpu.make_async_remote_copy(
            src_ref=src,
            dst_ref=dst,
            send_sem=self.send_sem.at[index],
            recv_sem=self.recv_sem.at[index],
            device_id=device,
            device_id_type=MESH,
        )
        copy.start()
        self.made[key] = copy

    def arrived(self, key):
        if key not in self.waited:
            self.waited.add(key)
            self.made[key].wait_recv()

    def drain(self):
        for copy in self.made.values():
            copy.wait_send()


def gather_kernel(fs_count, tp_count, xl, xe, wg, wu, out_xl, out_xe, out_wg, out_wu, ssem, rsem):
    z, x, tp, n = place(fs_count)
    bits = bits_of(tp_count)
    rows, half = wg.shape[0], wg.shape[1] // 2
    tokens = xl.shape[0]
    ahead = (lax.rem(z + 1, n) * 2 + x, tp)
    behind = (lax.rem(z + n - 1, n) * 2 + x, tp)
    beside = (z * 2 + 1 - x, tp)
    greet([ahead, behind, beside] + [(z * 2 + x, flip(tp, bit)) for bit in bits])
    copies = Copies(ssem, rsem)

    def block(offset, side):
        at = lax.rem(z + offset + n, n) * 2 + side
        return pl.ds(pl.multiple_of(at * rows, rows), rows)

    def own_tokens(mask):
        return pl.ds(pl.multiple_of(flips(tp, mask, bits) * tokens, tokens), tokens)

    lanes = {"f": pl.ds(0, half), "b": pl.ds(half, half)}
    towards = {"f": ahead, "b": behind}
    mine = block(0, x)
    for name, src, out in (("e", xe, out_xe), ("l", xl, out_xl)):
        for bit in bits[::-1]:
            copies.start((name, bit, 0), src, out.at[own_tokens(0)], (z * 2 + x, flip(tp, bit)))
    for way in "fb":
        copies.start(("up", way, 0), wu.at[:, lanes[way]], out_wu.at[mine, lanes[way]], towards[way])
    copies.start("gate_beside", wg, out_wg.at[mine], beside)
    for way in "fb":
        copies.start(("gate", way, 0), wg.at[:, lanes[way]], out_wg.at[mine, lanes[way]], towards[way])
    copies.start("up_beside", wu, out_wu.at[mine], beside)
    out_wu[mine, :] = wu[...]
    out_wg[mine, :] = wg[...]
    out_xe[own_tokens(0), :] = xe[...]
    out_xl[own_tokens(0), :] = xl[...]

    def ring(name, out, side, way, step):
        copies.arrived((name, way, step))
        offset = -1 - step if way == "f" else 1 + step
        at = (block(offset, side), lanes[way])
        if step < n - 2:
            copies.start((name, way, step + 1), out.at[at], out.at[at], towards[way])
        return at

    def spread(step):
        for way in "fb":
            at = ring("up", out_wu, x, way, step)
            copies.start(("up_beside", way, step), out_wu.at[at], out_wu.at[at], beside)

    spread(0)
    copies.arrived("gate_beside")
    other = block(0, 1 - x)
    for way in "fb":
        at = (other, lanes[way])
        copies.start(("pair", way, 0), out_wg.at[at], out_wg.at[at], towards[way])
    for step in range(n - 1):
        if step:
            spread(step)
        for way in "fb":
            ring("gate", out_wg, x, way, step)
        if step == 0:
            for place_of, bit in enumerate(bits[::-1]):
                held = bits[::-1][:place_of]
                for mask in range(1, tp_count):
                    if any(mask & b for b in bits if b not in held):
                        continue
                    for name, out in (("e", out_xe), ("l", out_xl)):
                        top = mask & -mask
                        copies.arrived((name, top, mask ^ top))
                        at = own_tokens(mask)
                        copies.start((name, bit, mask), out.at[at], out.at[at], (z * 2 + x, flip(tp, bit)))
        for way in "fb":
            ring("pair", out_wg, 1 - x, way, step)
    copies.arrived("up_beside")
    for step in range(n - 1):
        for way in "fb":
            copies.arrived(("up_beside", way, step))
    for name in "el":
        for mask in range(1, tp_count):
            low = mask & -mask
            copies.arrived((name, low, mask ^ low))
    copies.drain()


def add(a, b):
    return a.astype(F32) + b.astype(F32)


def reduce_kernel(
    fs_count, tp_count, dg, du, dx, gs, us, out_g, out_u, out_x,
    slots_a, last_a, slots_b, slots_c, slots_x, ssem, rsem,
):
    z, x, tp, n = place(fs_count)
    bits = bits_of(tp_count)
    rows, half = gs.shape[0], gs.shape[1] // 2
    tokens = out_x.shape[0]
    ahead = (lax.rem(z + 1, n) * 2 + x, tp)
    behind = (lax.rem(z + n - 1, n) * 2 + x, tp)
    beside = (z * 2 + 1 - x, tp)
    greet([ahead, behind, beside] + [(z * 2 + x, flip(tp, bit)) for bit in bits])
    copies = Copies(ssem, rsem)
    lanes = {"f": pl.ds(0, half), "b": pl.ds(half, half)}
    towards = {"f": ahead, "b": behind}

    def pair(offset):
        at = lax.rem(z + offset + n, n)
        return pl.ds(pl.multiple_of(at * 2 * rows, 2 * rows), 2 * rows)

    def block(offset, side):
        at = lax.rem(z + offset + n, n) * 2 + side
        return pl.ds(pl.multiple_of(at * rows, rows), rows)

    def chunk(mask):
        return pl.ds(pl.multiple_of(flips(tp, mask, bits) * tokens, tokens), tokens)

    for way in "fb":
        at = (pair(-1 if way == "f" else 1), lanes[way])
        copies.start(("a", way, 0), dg.at[at], slots_a.at[0, :, lanes[way]], towards[way])
    order = []
    for step in range(n):
        for offset in ((-1 - step) % n, (1 + step) % n):
            if offset not in order:
                order.append(offset)
    for offset in order:
        copies.start(("b", offset), du.at[block(offset, 1 - x)], slots_b.at[offset], beside)

    def above(bit):
        return [m for m in range(0, tp_count, 2 * bit)]

    slot_of = {}
    for bit in bits:
        for mask in above(bit):
            slot_of[bit, mask] = len(slot_of)
    first = bits[0]
    for mask in above(first)[::-1]:
        copies.start(("x", first, mask), dx.at[chunk(mask | first)], slots_x.at[slot_of[first, mask]], (z * 2 + x, flip(tp, first)))

    def sum_x(bit, mask):
        total = dx[chunk(mask), :].astype(F32)
        for b in bits:
            if b <= bit:
                total = total + slots_x[slot_of[b, mask]].astype(F32)
        return total

    for level in range(1, len(bits)):
        bit = bits[level]
        for mask in above(bit)[::-1]:
            sent = mask | bit
            for b in bits[:level]:
                if b == bits[level - 1]:
                    copies.arrived(("x", b, sent))
            slot = slots_x.at[slot_of[bits[level - 1], sent]]
            slot[...] = sum_x(bits[level - 1], sent).astype(BF16)
            copies.start(("x", bit, mask), slot, slots_x.at[slot_of[bit, mask]], (z * 2 + x, flip(tp, bit)))

    ready = set()

    def beside_sum(offset):
        offset = offset % n
        if offset not in ready:
            ready.add(offset)
            copies.arrived(("b", offset))
            if offset:
                slots_b[offset] = add(slots_b[offset], du[block(offset, x), :]).astype(BF16)
        return offset

    for way in "fb":
        offset = beside_sum(-1 if way == "f" else 1)
        copies.start(("c", way, 0), slots_b.at[offset, :, lanes[way]], slots_c.at[0, :, lanes[way]], towards[way])
    for step in range(n - 1):
        for way in "fb":
            copies.arrived(("a", way, step))
            if step < n - 2:
                at = (pair(-2 - step if way == "f" else 2 + step), lanes[way])
                slots_a[step, :, lanes[way]] = add(slots_a[step, :, lanes[way]], dg[at]).astype(BF16)
                copies.start(("a", way, step + 1), slots_a.at[step, :, lanes[way]], slots_a.at[step + 1, :, lanes[way]], towards[way])
            else:
                there = pl.ds(pl.multiple_of((1 - x) * rows, rows), rows)
                at = (there, lanes[way])
                slots_a[step, there, lanes[way]] = add(
                    slots_a[step, there, lanes[way]], dg[block(0, 1 - x), lanes[way]]
                ).astype(BF16)
                copies.start(("last", way), slots_a.at[step, there, lanes[way]], last_a.at[:, lanes[way]], beside)
        for way in "fb":
            offset = beside_sum(-2 - step if way == "f" else 2 + step)
            copies.arrived(("c", way, step))
            if step < n - 2:
                slots_c[step, :, lanes[way]] = add(
                    slots_c[step, :, lanes[way]], slots_b[offset, :, lanes[way]]
                ).astype(BF16)
                copies.start(("c", way, step + 1), slots_c.at[step, :, lanes[way]], slots_c.at[step + 1, :, lanes[way]], towards[way])
    for b in bits:
        copies.arrived(("x", b, 0))
    out_x[...] = sum_x(bits[-1], 0).astype(BF16)
    out_u[...] = us[...] + (
        add(slots_b[0], du[block(0, x), :]) + slots_c[n - 2].astype(F32)
    )
    here = pl.ds(pl.multiple_of(x * rows, rows), rows)
    for way in "fb":
        copies.arrived(("last", way))
    out_g[...] = gs[...] + (
        add(slots_a[n - 2, here, :], dg[block(0, x), :]) + last_a[...].astype(F32)
    )
    copies.drain()


def vmem(count):
    return [pl.BlockSpec(memory_space=pltpu.VMEM)] * count


def local(fs_count, tp_count, x_late, x_early, d_hidden, w_gate, w_up, gate_sum, up_sum):
    n = fs_count // 2
    tokens, width = x_early.shape
    rows, cols = w_gate.shape
    full = jax.ShapeDtypeStruct((fs_count * rows, cols), BF16)
    group = jax.ShapeDtypeStruct((tp_count * tokens, width), BF16)
    count = 2 * (tp_count - 1) + 8 * (n - 1) + 2
    rows_late, rows_early, full_gate, full_up = pl.pallas_call(
        functools.partial(gather_kernel, fs_count, tp_count),
        out_shape=(group, group, full, full),
        in_specs=vmem(4),
        out_specs=tuple(vmem(4)),
        scratch_shapes=[pltpu.SemaphoreType.DMA((count,)), pltpu.SemaphoreType.DMA((count,))],
        compiler_params=pltpu.CompilerParams(collective_id=0, has_side_effects=True),
        name="gather",
    )(x_late, x_early, w_gate, w_up)

    contract = (((1,), (1,)), ((), ()))
    tokens_dim = (((0,), (0,)), ((), ()))
    gate_early = jnp.dot(rows_early, full_gate, preferred_element_type=F32)
    up_early = jnp.dot(rows_early, full_up, preferred_element_type=F32)
    s = jax.nn.sigmoid(gate_early)
    cotangent = d_hidden.astype(F32)
    d_gate = (cotangent * up_early * s * (1.0 + gate_early * (1.0 - s))).astype(BF16)
    d_up = (cotangent * gate_early * s).astype(BF16)
    grad_gate = lax.dot_general(rows_early, d_gate, tokens_dim, preferred_element_type=F32).astype(BF16)
    grad_up = lax.dot_general(rows_early, d_up, tokens_dim, preferred_element_type=F32).astype(BF16)
    partial_value = lax.dot_general(d_gate, full_gate, contract, preferred_element_type=F32)
    partial_value = partial_value + lax.dot_general(d_up, full_up, contract, preferred_element_type=F32)
    partial_value = partial_value.astype(BF16)
    gate_late = jnp.dot(rows_late, full_gate, preferred_element_type=F32)
    up_late = jnp.dot(rows_late, full_up, preferred_element_type=F32)
    hidden_late = (gate_late * jax.nn.sigmoid(gate_late) * up_late).astype(BF16)

    count = (tp_count - 1) + 4 * (n - 1) + n + 2
    gate_out, up_out, grad_input = pl.pallas_call(
        functools.partial(reduce_kernel, fs_count, tp_count),
        out_shape=(
            jax.ShapeDtypeStruct(gate_sum.shape, F32),
            jax.ShapeDtypeStruct(up_sum.shape, F32),
            jax.ShapeDtypeStruct(x_early.shape, BF16),
        ),
        in_specs=vmem(5),
        out_specs=tuple(vmem(3)),
        scratch_shapes=[
            pltpu.VMEM((n - 1, 2 * rows, cols), BF16),
            pltpu.VMEM((rows, cols), BF16),
            pltpu.VMEM((n, rows, cols), BF16),
            pltpu.VMEM((n - 1, rows, cols), BF16),
            pltpu.VMEM((tp_count - 1, tokens, width), BF16),
            pltpu.SemaphoreType.DMA((count,)),
            pltpu.SemaphoreType.DMA((count,)),
        ],
        compiler_params=pltpu.CompilerParams(collective_id=1, has_side_effects=True),
        name="reduce",
    )(grad_gate, grad_up, partial_value, gate_sum, up_sum)
    return (hidden_late, grad_input, gate_out, up_out)


def solution(mesh):
    return jax.shard_map(
        functools.partial(local, mesh.shape["fs"], mesh.shape["tp"]),
        mesh=mesh,
        in_specs=(
            P(("fs", "tp"), None),
            P(("fs", "tp"), None),
            P("fs", "tp"),
            P("fs", "tp"),
            P("fs", "tp"),
            P("fs", "tp"),
            P("fs", "tp"),
        ),
        out_specs=(P("fs", "tp"), P(("fs", "tp"), None), P("fs", "tp"), P("fs", "tp")),
        check_vma=False,
    )
```

```python
import functools

import jax
import jax.numpy as jnp
from jax import lax
from jax.experimental import pallas as pl
from jax.experimental.pallas import tpu as pltpu
from jax.sharding import PartitionSpec as P

MESH = pl.DeviceIdType.MESH
F32 = jnp.float32
BF16 = jnp.bfloat16


def place(fs_count):
    fs, tp = lax.axis_index("fs"), lax.axis_index("tp")
    return lax.div(fs, 2), lax.rem(fs, 2), tp, fs_count // 2


def bits_of(tp_count):
    return [1 << b for b in range(tp_count.bit_length() - 1)]


def flip(tp, bit):
    return jnp.where(lax.rem(lax.div(tp, bit), 2) == 0, tp + bit, tp - bit)


def flips(tp, mask, bits):
    for bit in bits:
        if mask & bit:
            tp = flip(tp, bit)
    return tp


class Copies:
    def __init__(self, send_sem, recv_sem):
        self.send_sem, self.recv_sem = send_sem, recv_sem
        self.index, self.sent = {}, []

    def number(self, key):
        return self.index.setdefault(key, len(self.index))

    def make(self, key, src, dst, device):
        at = self.number(key) if isinstance(key, tuple) else key
        return pltpu.make_async_remote_copy(
            src_ref=src, dst_ref=dst, send_sem=self.send_sem.at[at], recv_sem=self.recv_sem.at[at],
            device_id=device, device_id_type=MESH,
        )

    def start(self, key, src, dst, device, when=None):
        copy = self.make(key, src, dst, device)
        self.sent.append((copy, when))
        under(when, copy.start)

    def arrived(self, key, dst, device):
        self.make(key, dst, dst, device).wait_recv()

    def drain(self):
        for copy, when in self.sent:
            under(when, copy.wait_send)


def under(when, action):
    if when is None:
        action()
    else:
        pl.when(when)(action)


def neighbours(z, x, tp, n, bits):
    up = (jnp.minimum(z + 1, n - 1) * 2 + x, tp)
    down = (jnp.maximum(z - 1, 0) * 2 + x, tp)
    beside = (z * 2 + 1 - x, tp)
    barrier = pltpu.get_barrier_semaphore()

    def greet(device):
        pl.semaphore_signal(barrier, inc=1, device_id=device, device_id_type=MESH)

    pl.when(z < n - 1)(lambda: greet(up))
    pl.when(z > 0)(lambda: greet(down))
    for device in [beside] + [(z * 2 + x, flip(tp, bit)) for bit in bits]:
        greet(device)
    ends = jnp.where(z < n - 1, 1, 0) + jnp.where(z > 0, 1, 0)
    pl.semaphore_wait(barrier, 1 + len(bits) + ends)
    return up, down, beside


def gather_kernel(fs_count, tp_count, early, xl, xe, w, out_xl, out_xe, out_w, ssem, rsem):
    z, x, tp, n = place(fs_count)
    bits = bits_of(tp_count)
    rows, cols = w.shape
    tokens = xl.shape[0]
    up, down, beside = neighbours(z, x, tp, n, bits)
    copies = Copies(ssem, rsem)
    first = pl.ds(0, early)
    size = (cols - early) // 256 * 128
    parts = (pl.ds(early, size), pl.ds(early + size, cols - early - size))

    def chunk(at, side):
        return pl.ds(pl.multiple_of((at * 2 + side) * rows, rows), rows)

    def pair(at):
        return pl.ds(pl.multiple_of(at * 2 * rows, 2 * rows), 2 * rows)

    def own_tokens(mask):
        return pl.ds(pl.multiple_of(flips(tp, mask, bits) * tokens, tokens), tokens)

    ways = (("u", up, z < n - 1), ("d", down, z > 0))
    mine = chunk(z, x)
    copies.start(("first",), w.at[:, first], out_w.at[mine, first], beside)
    for index, rest in enumerate(parts):
        for name, device, when in ways:
            copies.start((name, 0, index), w.at[:, rest], out_w.at[mine, rest], device, when)
    for name, src, out in (("e", xe, out_xe), ("l", xl, out_xl)):
        for bit in bits[::-1]:
            copies.start((name, bit, 0), src, out.at[own_tokens(0)], (z * 2 + x, flip(tp, bit)))
    for index, rest in enumerate(parts):
        copies.start(("beside", index), w.at[:, rest], out_w.at[mine, rest], beside)
    out_w[mine, :] = w[...]
    out_xe[own_tokens(0), :] = xe[...]
    out_xl[own_tokens(0), :] = xl[...]

    def origin(name, step):
        at = z - 1 - step if name == "u" else z + 1 + step
        has = at >= 0 if name == "u" else at <= n - 1
        return jnp.clip(at, 0, n - 1), has

    sides = []
    for step in range(n - 1):
        for index, rest in enumerate(parts):
            for name, device, when in ways:
                at, has = origin(name, step)
                ref = out_w.at[chunk(at, x), rest]
                pl.when(has)(lambda: copies.arrived((name, step, index), ref, device))
                copies.start((name, step + 1, index), ref, ref, device, has & when)
                copies.start(("beside", name, step, index), ref, ref, beside, has)
                sides.append((("beside", name, step, index), out_w.at[chunk(at, 1 - x), rest], has))
        if step == 0:
            theirs = out_w.at[chunk(z, 1 - x), first]
            copies.arrived(("first",), theirs, beside)
            both = out_w.at[pair(z), first]
            for name, device, when in ways:
                copies.start(("pair" + name, 0), both, both, device, when)
            for level, bit in enumerate(bits[::-1]):
                for mask in range(1, tp_count):
                    top = mask & -mask
                    if top > bit:
                        for out, key in ((out_xe, "e"), (out_xl, "l")):
                            ref = out.at[own_tokens(mask)]
                            if top == bit * 2:
                                copies.arrived((key, top, mask ^ top), ref, beside)
                            copies.start((key, bit, mask), ref, ref, (z * 2 + x, flip(tp, bit)))
    for step in range(n - 1):
        for name, device, when in ways:
            at, has = origin(name, step)
            ref = out_w.at[pair(at), first]
            pl.when(has)(lambda: copies.arrived(("pair" + name, step), ref, device))
            copies.start(("pair" + name, step + 1), ref, ref, device, has & when)
    for index, rest in enumerate(parts):
        copies.arrived(("beside", index), out_w.at[chunk(z, 1 - x), rest], beside)
    for key, ref, has in sides:
        pl.when(has)(lambda: copies.arrived(key, ref, beside))
    for out, key in ((out_xe, "e"), (out_xl, "l")):
        for mask in range(1, tp_count):
            if mask & 1:
                copies.arrived((key, 1, mask ^ 1), out.at[own_tokens(mask)], beside)
    copies.drain()


def add(a, b):
    return a.astype(F32) + b.astype(F32)


def reduce_kernel(
    fs_count, tp_count, early, dw, dx, gs, us, out_g, out_u, out_x,
    slots_p, last, slots_b, slots_z, slots_x, ssem, rsem,
):
    z, x, tp, n = place(fs_count)
    bits = bits_of(tp_count)
    rows, cols = gs.shape
    tokens = out_x.shape[0]
    up, down, beside = neighbours(z, x, tp, n, bits)
    copies = Copies(ssem, rsem)
    first, rest = pl.ds(0, early), pl.ds(early, 2 * cols - early)

    def chunk(at, side):
        return pl.ds(pl.multiple_of((at * 2 + side) * rows, rows), rows)

    def tp_chunk(mask):
        return pl.ds(pl.multiple_of(flips(tp, mask, bits) * tokens, tokens), tokens)

    near = jnp.where(z < n // 2, 0, 1)

    def way(d):
        to, back = z + 1 - 2 * d, z - 1 + 2 * d
        return d, (jnp.clip(to, 0, n - 1) * 2 + x, tp), (back >= 0) & (back <= n - 1)

    ways = (way(near), way(1 - near))

    def target_of(d, step):
        target = jnp.where(d == 0, n - 1 - step, step)
        return target, (1 - 2 * d) * (target - z) > 0

    def hop(name, d, step):
        return bases[name] + d * (n - 1) + step

    for k in range(n):
        copies.number(("b", k))
    bases = {}
    for name in "pz":
        bases[name] = len(copies.index)
        for k in range(2 * (n - 1)):
            copies.number((name, k))

    def pairs(step):
        for d, device, from_behind in ways:
            target, passes = target_of(d, step)
            own = dw.at[pl.ds(pl.multiple_of(target * 2 * rows, 2 * rows), 2 * rows), first]
            slot = slots_p.at[d, step]

            def pass_on(own=own, slot=slot, key=hop("p", d, step), device=device):
                copies.arrived(key, slot, device)
                slot[...] = add(slot[...], own[...]).astype(BF16)

            pl.when(passes & from_behind)(pass_on)
            copies.start(hop("p", d, step), slot, slot, device, passes & from_behind)
            start = copies.make(hop("p", d, step), own, slot, device)
            edge = passes & jnp.logical_not(from_behind)
            pl.when(edge)(start.start)
            edges.append((start, edge))

    edges = []
    for k in range(n):
        low = n - 1 - k
        low = jnp.where(low <= z, low - 1, low)
        high = jnp.where(k >= z, k + 1, k)
        at = z if k == n - 1 else jnp.where(z < n // 2, low, high)
        at = jnp.clip(at, 0, n - 1)
        copies.start(at, dw.at[chunk(at, 1 - x), rest], slots_b.at[at], beside)
    pairs(0)

    def above(bit):
        return [m for m in range(0, tp_count, 2 * bit)]

    slot_of = {}
    for bit in bits:
        for mask in above(bit):
            slot_of[bit, mask] = len(slot_of)

    def send_x(bit, mask, src):
        copies.start(("x", bit, mask), src, slots_x.at[slot_of[bit, mask]], (z * 2 + x, flip(tp, bit)))

    def recv_x(bit, mask):
        copies.arrived(("x", bit, mask), slots_x.at[slot_of[bit, mask]], beside)

    def sum_x(bit, mask):
        total = dx[tp_chunk(mask), :].astype(F32)
        for b in bits:
            if b <= bit:
                total = total + slots_x[slot_of[b, mask]].astype(F32)
        return total

    for mask in above(bits[0])[::-1]:
        send_x(bits[0], mask, dx.at[tp_chunk(mask | bits[0])])
    for step in range(1, n - 1):
        pairs(step)
    for level in range(1, len(bits)):
        bit, before = bits[level], bits[level - 1]
        for mask in above(bit)[::-1]:
            sent = mask | bit
            recv_x(before, sent)
            slot = slots_x.at[slot_of[before, sent]]
            slot[...] = sum_x(before, sent).astype(BF16)
            send_x(bit, mask, slot)

    def beside_sum(target):
        copies.arrived(target, slots_b.at[target], beside)
        slots_b[target] = add(slots_b[target], dw[chunk(target, x), rest]).astype(BF16)

    def chunks(step):
        for d, device, from_behind in ways:
            target, passes = target_of(d, step)
            slot = slots_z.at[d, step]

            def pass_on(slot=slot, key=hop("z", d, step), device=device, target=target):
                copies.arrived(key, slot, device)
                slot[...] = add(slot[...], slots_b[target]).astype(BF16)

            pl.when(passes)(lambda: beside_sum(target))
            pl.when(passes & from_behind)(pass_on)
            copies.start(hop("z", d, step), slot, slot, device, passes & from_behind)
            start = copies.make(hop("z", d, step), slots_b.at[target], slot, device)
            edge = passes & jnp.logical_not(from_behind)
            pl.when(edge)(start.start)
            edges.append((start, edge))

    chunks(0)
    theirs = pl.ds(pl.multiple_of((1 - x) * rows, rows), rows)
    ours = pl.ds(pl.multiple_of(x * rows, rows), rows)
    own_pair = dw.at[pl.ds(pl.multiple_of(z * 2 * rows, 2 * rows), 2 * rows), first]
    last[...] = own_pair[...].astype(F32)
    for d, from_behind in ((0, z > 0), (1, z < n - 1)):
        for step in range(n - 1):
            target = n - 1 - step if d == 0 else step

            def take(d=d, step=step):
                copies.arrived(hop("p", d, step), slots_p.at[d, step], beside)
                last[...] = last[...] + slots_p[d, step].astype(F32)

            pl.when((z == target) & from_behind)(take)
    slots_p[0, n - 1] = last[...].astype(BF16)
    copies.start(("last",), slots_p.at[0, n - 1, theirs, :], slots_p.at[1, n - 1, pl.ds(0, rows), :], beside)
    for step in range(1, n - 1):
        chunks(step)
    for b in bits:
        recv_x(b, 0)
    out_x[...] = sum_x(bits[-1], 0).astype(BF16)
    copies.arrived(z, slots_b.at[z], beside)
    left, right = pl.ds(0, cols - early), pl.ds(cols - early, cols)
    tail = pl.ds(early, cols - early)
    whole = add(slots_b[z], dw[chunk(z, x), rest])
    out_g[:, tail] = gs[:, tail] + whole[:, : cols - early]
    out_u[...] = us[...] + whole[:, cols - early :]
    copies.arrived(("last",), slots_p.at[1, n - 1, pl.ds(0, rows), :], beside)
    out_g[:, first] = gs[:, first] + (last[ours, :] + slots_p[1, n - 1, pl.ds(0, rows), :].astype(F32))
    for d, from_behind in ((0, z > 0), (1, z < n - 1)):
        for step in range(n - 1):
            target = n - 1 - step if d == 0 else step

            def take(d=d, step=step):
                slot = slots_z.at[d, step]
                copies.arrived(hop("z", d, step), slot, beside)
                out_g[:, tail] += slot[:, left].astype(F32)
                out_u[...] += slot[:, right].astype(F32)

            pl.when((z == target) & from_behind)(take)
    copies.sent += edges
    copies.drain()


def vmem(count):
    return [pl.BlockSpec(memory_space=pltpu.VMEM)] * count


def local(fs_count, tp_count, x_late, x_early, d_hidden, w_gate, w_up, gate_sum, up_sum):
    n = fs_count // 2
    tokens, width = x_early.shape
    rows, cols = w_gate.shape
    early = max(128, cols // 3 // 128 * 128)
    full = jax.ShapeDtypeStruct((fs_count * rows, 2 * cols), BF16)
    group = jax.ShapeDtypeStruct((tp_count * tokens, width), BF16)
    weights = jnp.concatenate([w_gate, w_up], axis=1)
    count = 2 * (tp_count - 1) + 10 * n + 3
    rows_late, rows_early, full_w = pl.pallas_call(
        functools.partial(gather_kernel, fs_count, tp_count, early),
        out_shape=(group, group, full),
        in_specs=vmem(3),
        out_specs=tuple(vmem(3)),
        scratch_shapes=[pltpu.SemaphoreType.DMA((count,)), pltpu.SemaphoreType.DMA((count,))],
        compiler_params=pltpu.CompilerParams(collective_id=0, has_side_effects=True),
        name="gather",
    )(x_late, x_early, weights)

    contract = (((1,), (1,)), ((), ()))
    tokens_dim = (((0,), (0,)), ((), ()))
    pre = jnp.dot(rows_early, full_w, preferred_element_type=F32)
    gate_early, up_early = pre[:, :cols], pre[:, cols:]
    s = jax.nn.sigmoid(gate_early)
    cotangent = d_hidden.astype(F32)
    d_gate = (cotangent * up_early * s * (1.0 + gate_early * (1.0 - s))).astype(BF16)
    d_up = (cotangent * gate_early * s).astype(BF16)
    d_both = jnp.concatenate([d_gate, d_up], axis=1)
    grad_w = lax.dot_general(rows_early, d_both, tokens_dim, preferred_element_type=F32).astype(BF16)
    partial_value = lax.dot_general(d_both, full_w, contract, preferred_element_type=F32).astype(BF16)
    pre = jnp.dot(rows_late, full_w, preferred_element_type=F32)
    gate_late, up_late = pre[:, :cols], pre[:, cols:]
    hidden_late = (gate_late * jax.nn.sigmoid(gate_late) * up_late).astype(BF16)

    count = (tp_count - 1) + 4 * (n - 1) + n + 1
    gate_out, up_out, grad_input = pl.pallas_call(
        functools.partial(reduce_kernel, fs_count, tp_count, early),
        out_shape=(
            jax.ShapeDtypeStruct(gate_sum.shape, F32),
            jax.ShapeDtypeStruct(up_sum.shape, F32),
            jax.ShapeDtypeStruct(x_early.shape, BF16),
        ),
        in_specs=vmem(4),
        out_specs=tuple(vmem(3)),
        scratch_shapes=[
            pltpu.VMEM((2, n, 2 * rows, early), BF16),
            pltpu.VMEM((2 * rows, early), F32),
            pltpu.VMEM((n, rows, 2 * cols - early), BF16),
            pltpu.VMEM((2, n - 1, rows, 2 * cols - early), BF16),
            pltpu.VMEM((tp_count - 1, tokens, width), BF16),
            pltpu.SemaphoreType.DMA((count,)),
            pltpu.SemaphoreType.DMA((count,)),
        ],
        compiler_params=pltpu.CompilerParams(collective_id=1, has_side_effects=True),
        name="reduce",
    )(grad_w, partial_value, gate_sum, up_sum)
    return (hidden_late, grad_input, gate_out, up_out)


def solution(mesh):
    return jax.shard_map(
        functools.partial(local, mesh.shape["fs"], mesh.shape["tp"]),
        mesh=mesh,
        in_specs=(
            P(("fs", "tp"), None),
            P(("fs", "tp"), None),
            P("fs", "tp"),
            P("fs", "tp"),
            P("fs", "tp"),
            P("fs", "tp"),
            P("fs", "tp"),
        ),
        out_specs=(P("fs", "tp"), P(("fs", "tp"), None), P("fs", "tp"), P("fs", "tp")),
        check_vma=False,
    )
```
